32 devices in a mesh: tp: 8 (over z, x), dp: 4 (over y, core).
Axes of the slice: x: 2, y: 2, z: 4, core: 2. Of those that a mesh axis runs over, the one named last changes fastest.
Arguments:
- tokens: bfloat16 [128, 4096], P('tp', 'dp'), may hold values from -6 to 6
- query_weight: bfloat16 [2, 4096, 2048], P(None, 'dp', 'tp'), may hold values from -0.09375 to 0.09375
- key_weight: bfloat16 [2, 4096, 2048], P(None, 'dp', 'tp'), may hold values from -0.09375 to 0.09375
- value_weight: bfloat16 [2, 4096, 2048], P(None, 'dp', 'tp'), may hold values from -0.09375 to 0.09375
- outgate_weight: bfloat16 [2, 4096, 2048], P(None, 'dp', 'tp'), may hold values from -0.09375 to 0.09375
- igate_weight: bfloat16 [2, 4096, 16], replicated, may hold values from -0.09375 to 0.09375
- fgate_weight: bfloat16 [2, 4096, 16], replicated, may hold values from -0.09375 to 0.09375
- norm_gain: float32 [2, 4096], P(None, 'dp'), may hold values from 0.1 to 1.9
- head_gain: float32 [2, 2048], P(None, 'tp'), may hold values from 0.1 to 1.9
- proj_weight: bfloat16 [2, 2048, 4096], P(None, 'tp', 'dp'), may hold values from -0.125 to 0.125
- cell_state: float32 [2, 128, 16, 128, 128], P(None, 'dp', 'tp'), may hold values from -1.8 to 1.8
- normer_state: float32 [2, 128, 16, 128], P(None, 'dp', 'tp'), may hold values from -1.8 to 1.8
- stab_state: float32 [2, 128, 16], P(None, 'dp', 'tp'), may hold values from -4 to 4
Outputs:
- final_rows: bfloat16 [128, 4096], P('tp', 'dp')
- cell_out: float32 [2, 128, 16, 128, 128], P(None, 'dp', 'tp')
- normer_out: float32 [2, 128, 16, 128], P(None, 'dp', 'tp')
- stab_out: float32 [2, 128, 16], P(None, 'dp', 'tp')
The draws below stay inside these ranges and needn't reach their ends.
All inputs are finite; a program needn't handle non-finite values.
Results may differ from the reference program's by a relative error of at most 0.012.
The reference program's roundings to bfloat16 on the way count: a program that leaves them out, or rounds other values in their place, can miss the bound.
Values may be sent and summed in bfloat16 or wider, within the bound.
A program may use at most 64 MiB of HBM per device.

```python
import jax
import jax.numpy as jnp
from jax import lax

D = 4096
HEADS = 16
DH = 128
BLOCKS = 2
INNER = 2048
BATCH = 128


def block_levels(own_key, dims, shards, least, top_value):
    def one(axis_at, shards_of):
        draws = jax.random.uniform(jax.random.fold_in(jax.random.fold_in(own_key, 6), axis_at), (shards_of,), jnp.float32, least / len(shards), top_value / len(shards))
        return jnp.repeat(jnp.exp(draws), dims[axis_at] // shards_of).reshape((-1,) + (1,) * (len(dims) - axis_at - 1))

    gain = one(*shards[0])
    for cut in shards[1:]:
        gain = gain * one(*cut)
    return gain


def centred(key, extent, deviation, bound, split=(), held_as=jnp.bfloat16):
    entries = deviation * jax.random.normal(key, extent, jnp.float32)
    if split:
        entries = entries * block_levels(key, extent, split, -0.22, 0.18)
    return jnp.clip(entries, -bound, bound).astype(held_as)


def setup_inputs(seed: int = 0) -> dict:
    key_of = jax.random.split(jax.random.key(seed), 14)
    return {
        "tokens": centred(key_of[0], (BATCH, D), 1.0, 6.0, ((0, 8), (1, 4))),
        "query_weight": centred(key_of[1], (BLOCKS, D, INNER), D ** -0.5, 0.09375, ((1, 4), (2, 8))),
        "key_weight": centred(key_of[2], (BLOCKS, D, INNER), D ** -0.5, 0.09375, ((1, 4), (2, 8))),
        "value_weight": centred(key_of[3], (BLOCKS, D, INNER), D ** -0.5, 0.09375, ((1, 4), (2, 8))),
        "outgate_weight": centred(key_of[4], (BLOCKS, D, INNER), D ** -0.5, 0.09375, ((1, 4), (2, 8))),
        "igate_weight": centred(key_of[5], (BLOCKS, D, HEADS), D ** -0.5, 0.09375),
        "fgate_weight": centred(key_of[6], (BLOCKS, D, HEADS), D ** -0.5, 0.09375),
        "norm_gain": jnp.clip(1.0 + 0.18 * jax.random.normal(key_of[7], (BLOCKS, D), jnp.float32), 0.1, 1.9),
        "head_gain": jnp.clip(1.0 + 0.18 * jax.random.normal(key_of[8], (BLOCKS, INNER), jnp.float32), 0.1, 1.9),
        "proj_weight": centred(key_of[9], (BLOCKS, INNER, D), INNER ** -0.5, 0.125, ((1, 8), (2, 4))),
        "cell_state": centred(key_of[10], (BLOCKS, BATCH, HEADS, DH, DH), 0.3, 1.8, ((1, 4), (2, 8)), jnp.float32),
        "normer_state": centred(key_of[11], (BLOCKS, BATCH, HEADS, DH), 0.3, 1.8, ((1, 4), (2, 8)), jnp.float32),
        "stab_state": centred(key_of[12], (BLOCKS, BATCH, HEADS), 1.0, 4.0, ((1, 4), (2, 8)), jnp.float32),
    }


EPSILON = 1e-06

def reference(tokens, query_weight, key_weight, value_weight, outgate_weight, igate_weight, fgate_weight, norm_gain, head_gain, proj_weight, cell_state, normer_state, stab_state):
    current = tokens
    batch_rows = tokens.shape[0]
    cell_list = []
    normer_list = []
    stab_list = []
    for layer_num in range(BLOCKS):
        as_float = current.astype(jnp.float32)
        inv_rms = lax.rsqrt(lax.optimization_barrier(jnp.mean(as_float * as_float, axis=1, keepdims=True)) + EPSILON)
        scaled = (as_float * norm_gain[layer_num].astype(jnp.float32)).astype(jnp.bfloat16)

        def product(weight):
            return jnp.dot(scaled, weight, preferred_element_type=jnp.float32) * inv_rms
        query_rows = product(query_weight[layer_num]).reshape(batch_rows, HEADS, DH)
        key_rows = (product(key_weight[layer_num]) * DH ** (-0.5)).reshape(batch_rows, HEADS, DH)
        value_rows = product(value_weight[layer_num]).reshape(batch_rows, HEADS, DH)
        outgate = product(outgate_weight[layer_num])
        igate = product(igate_weight[layer_num])
        forget = jax.nn.log_sigmoid(product(fgate_weight[layer_num]))
        prev_stab = stab_state[layer_num]
        new_stab = jnp.maximum(forget + prev_stab, igate)
        keep_rate = jnp.exp(forget + prev_stab - new_stab)
        write_rate = jnp.exp(igate - new_stab)
        new_cell = keep_rate[..., None, None] * cell_state[layer_num] + write_rate[..., None, None] * value_rows[..., :, None] * key_rows[..., None, :]
        new_normer = keep_rate[..., None] * normer_state[layer_num] + write_rate[..., None] * key_rows
        numerator = jnp.einsum('bhvd,bhd->bhv', new_cell, query_rows, precision=lax.Precision.HIGHEST)
        denominator = jnp.maximum(jnp.abs(lax.optimization_barrier(jnp.sum(new_normer * query_rows, axis=-1))), 1.0)
        readout = numerator / denominator[..., None]
        normed = readout * lax.rsqrt(lax.optimization_barrier(jnp.mean(readout * readout, axis=-1, keepdims=True)) + EPSILON)
        normed = normed * head_gain[layer_num].reshape(HEADS, DH)
        gated_out = (jax.nn.sigmoid(outgate) * normed.reshape(batch_rows, HEADS * DH)).astype(jnp.bfloat16)
        current = jnp.dot(gated_out, proj_weight[layer_num], preferred_element_type=jnp.float32).astype(jnp.bfloat16)
        cell_list.append(new_cell)
        normer_list.append(new_normer)
        stab_list.append(new_stab)
    return (current, jnp.stack(cell_list), jnp.stack(normer_list), jnp.stack(stab_list))
```

```python
import functools
import math

import jax
import jax.numpy as jnp
from jax import lax
from jax.experimental import pallas as pl
from jax.experimental.pallas import tpu as pltpu
from jax.sharding import PartitionSpec as P

EPSILON = 1e-06
F32 = jnp.float32
BF16 = jnp.bfloat16
MESH = pl.DeviceIdType.MESH


def split_axis(size):
    inner = max(f for f in range(1, math.isqrt(size) + 1) if size % f == 0)
    return size // inner, inner


def row_block(index, rows):
    return pl.ds(pl.multiple_of(index * rows, rows), rows)


def gate_dot(scaled, weight):
    return lax.dot_general(
        scaled, weight, (((1,), (1,)), ((), ())), preferred_element_type=F32
    )


def step_kernel(
    ntp,
    ndp,
    tokens,
    wq,
    wk,
    wv,
    wo,
    wig,
    wfg,
    norm_gain,
    head_gain,
    proj,
    cell,
    normer,
    stab,
    final_out,
    value_out,
    key_out,
    normer_out,
    aux_out,
    stab_out,
    w_buf,
    ig_buf,
    fg_buf,
    proj_buf,
    cell_buf,
    tok_sem,
    small_sem,
    gain_buf,
    head_buf,
    normer_buf,
    stab_buf,
    split_buf,
    current,
    partial,
    gates,
    pair_recv,
    pair_gate,
    pair_sum,
    pair_gsum,
    proj_recv,
    gate_recv,
    query_buf,
    read_buf,
    gated_all,
    out_part,
    out_stage,
    out_recv,
    load_sem,
    cell_sem,
    ag_send,
    ag_recv,
    pr_send,
    pr_recv,
    pg_send,
    pg_recv,
    rs_send,
    rs_recv,
    gt_send,
    gt_recv,
    gg_send,
    gg_recv,
    os_send,
    os_recv,
):
    blocks = wq.shape[0]
    width, inner = wq.shape[1], wq.shape[2]
    all_heads = wig.shape[1]
    seqs, heads, dh = cell.shape[1], cell.shape[2], cell.shape[3]
    rows = tokens.shape[0]
    t = lax.axis_index("tp")
    d = lax.axis_index("dp")
    outer, side = split_axis(ntp)
    z = t // side
    x = lax.rem(t, side)

    pair = 2 if ndp % 2 == 0 else 1
    ring = ndp // pair
    y = d // pair
    core = lax.rem(d, pair)

    tok_load = pltpu.make_async_copy(tokens, current.at[0, row_block(t, rows)], tok_sem)
    tok_load.start()
    small = [
        pltpu.make_async_copy(src, dst, small_sem.at[i])
        for i, (src, dst) in enumerate(
            (
                (norm_gain, gain_buf),
                (head_gain, head_buf),
                (normer, normer_buf),
                (stab, stab_buf),
            )
        )
    ]
    loads = []
    for b in range(blocks):
        for i, w in enumerate((wq, wk, wv, wo)):
            loads.append(pltpu.make_async_copy(w.at[b], w_buf.at[b, i], load_sem.at[b, i]))
        loads.append(
            pltpu.make_async_copy(
                wig.at[b, :, row_block(d, width)], ig_buf.at[b], load_sem.at[b, 4]
            )
        )
        loads.append(
            pltpu.make_async_copy(
                wfg.at[b, :, row_block(d, width)], fg_buf.at[b], load_sem.at[b, 5]
            )
        )
        loads.append(pltpu.make_async_copy(proj.at[b], proj_buf.at[b], load_sem.at[b, 6]))
    cell_loads = [
        pltpu.make_async_copy(cell.at[b], cell_buf.at[b], cell_sem.at[b]) for b in range(blocks)
    ]
    per_block = 7
    for b in range(blocks):
        for c in loads[b * per_block : (b + 1) * per_block]:
            c.start()
        cell_loads[b].start()
        if b == 0:
            for c in small:
                c.start()

    barrier = pltpu.get_barrier_semaphore()
    for k in range(1, ntp):
        pl.semaphore_signal(
            barrier, inc=1, device_id={"tp": lax.rem(t + k, ntp)}, device_id_type=MESH
        )
    for k in range(1, ndp):
        pl.semaphore_signal(
            barrier, inc=1, device_id={"dp": lax.rem(d + k, ndp)}, device_id_type=MESH
        )
    pl.semaphore_wait(barrier, ntp - 1 + ndp - 1)
    tok_load.wait()

    def split_cells(b):
        cell_loads[b].wait()

        def one(i, _):
            for h in range(heads):
                whole = cell_buf[b, i, h]
                high = whole.astype(BF16)
                split_buf[i, h, :, 0:dh] = high
                split_buf[i, h, :, dh : 2 * dh] = (whole - high.astype(F32)).astype(BF16)
            return 0

        lax.fori_loop(0, seqs, one, 0)

    def gather(b):
        buf = current.at[b]
        own_src = buf.at[row_block(t, rows)]

        def send(src, block, slot, dest):
            copy = pltpu.make_async_remote_copy(
                src_ref=src,
                dst_ref=buf.at[row_block(block, rows)],
                send_sem=ag_send.at[b, slot],
                recv_sem=ag_recv.at[b, slot],
                device_id={"tp": dest},
                device_id_type=MESH,
            )
            copy.start()
            return copy

        first, second = [], []
        for k in range(1, outer):
            dest = lax.rem(z + k, outer) * side + x
            first.append(send(own_src, t, k - 1, dest))
        for j in range(1, side):
            dest = z * side + lax.rem(x + j, side)
            second.append(send(own_src, t, outer - 1 + (j - 1) * outer, dest))
        if b == 0:
            split_cells(0)
            for c in small:
                c.wait()
        for k in range(1, outer):
            first[k - 1].wait_recv()
            block = lax.rem(z - k + outer, outer) * side + x
            for j in range(1, side):
                dest = z * side + lax.rem(x + j, side)
                second.append(
                    send(
                        buf.at[row_block(block, rows)],
                        block,
                        outer - 1 + (j - 1) * outer + k,
                        dest,
                    )
                )
        for c in second:
            c.wait_recv()
        for c in first + second:
            c.wait_send()

    for b in range(blocks):
        gather(b)
        for c in loads[b * per_block : (b + 1) * per_block]:
            c.wait()
        as_float = current[b].astype(F32)
        scaled = (as_float * gain_buf[b : b + 1, :]).astype(BF16)
        gates[b, :, 0:all_heads] = gate_dot(scaled, ig_buf[b])
        gates[b, :, all_heads : 2 * all_heads] = gate_dot(scaled, fg_buf[b])
        gates[b, :, 2 * all_heads : 2 * all_heads + 1] = jnp.sum(
            as_float * as_float, axis=1, keepdims=True
        )
        sends = []

        def send_rows(srcs, dsts, send_sems, recv_sems, slot, dest):
            started = []
            for src, dst, ss, rr in zip(srcs, dsts, send_sems, recv_sems):
                copy = pltpu.make_async_remote_copy(
                    src_ref=src,
                    dst_ref=dst,
                    send_sem=ss.at[b, slot],
                    recv_sem=rr.at[b, slot],
                    device_id={"dp": dest},
                    device_id_type=MESH,
                )
                copy.start()
                started.append(copy)
            sends.extend(started)
            return started

        for i in range(4):
            cols = slice(i * inner, (i + 1) * inner)
            partial[b, :, cols] = jnp.dot(scaled, w_buf[b, i], preferred_element_type=F32)
        paired = []
        if pair == 2:
            mate = y * pair + 1 - core
            for k in range(ring):
                slot = (k + 1) % ring
                block = row_block(lax.rem(y + slot, ring) * pair + 1 - core, seqs)
                paired.append(
                    (
                        slot,
                        send_rows(
                            (partial.at[b, block], gates.at[b, block]),
                            (pair_recv.at[b, slot], pair_gate.at[b, slot]),
                            (pr_send, pg_send),
                            (pr_recv, pg_recv),
                            slot,
                            mate,
                        ),
                    )
                )
        else:
            paired = [((k + 1) % ring, []) for k in range(ring)]
        arriving = []
        total = gate_sum = None
        for slot, copies in paired:
            for c in copies:
                c.wait_recv()
            dest = lax.rem(y + slot, ring) * pair + core
            block = row_block(dest, seqs)
            rows_sum, gsum = partial[b, block, :], gates[b, block, :]
            if copies:
                rows_sum = rows_sum + pair_recv[b, slot]
                gsum = gsum + pair_gate[b, slot]
            if slot == 0:
                total, gate_sum = rows_sum, gsum
            else:
                pair_sum[b, slot - 1] = rows_sum.astype(pair_sum.dtype)
                pair_gsum[b, slot - 1] = gsum
                arriving.append(
                    send_rows(
                        (pair_sum.at[b, slot - 1], pair_gsum.at[b, slot - 1]),
                        (proj_recv.at[b, slot - 1], gate_recv.at[b, slot - 1]),
                        (rs_send, gt_send),
                        (rs_recv, gt_recv),
                        slot - 1,
                        dest,
                    )
                )
        for k in range(ring - 1):
            for c in arriving[k]:
                c.wait_recv()
            total = total + proj_recv[b, k].astype(F32)
            gate_sum = gate_sum + gate_recv[b, k]
        own = row_block(d, seqs)
        inv_rms = lax.rsqrt(gate_sum[:, 2 * all_heads : 2 * all_heads + 1] / (width * ndp) + EPSILON)
        query = total[:, 0:inner] * inv_rms
        key = total[:, inner : 2 * inner] * inv_rms * (dh ** (-0.5))
        value = total[:, 2 * inner : 3 * inner] * inv_rms
        outgate = total[:, 3 * inner : 4 * inner] * inv_rms
        pre = gate_sum * inv_rms
        query_buf[...] = query
        key_out[b] = key
        def read_chunk(c, _):
            eight = pl.ds(pl.multiple_of(c * 8, 8), 8)
            sub = lax.broadcasted_iota(jnp.int32, (8, dh), 0)
            for h in range(heads):
                lanes = slice(h * dh, (h + 1) * dh)
                q8 = query_buf[eight, lanes]
                high = q8.astype(BF16)
                low = (q8 - high.astype(F32)).astype(BF16)
                high, low = jnp.concatenate([high, high], 1), jnp.concatenate([low, low], 1)
                lhs = jnp.concatenate([high, low], 0)
                acc = jnp.zeros((8, dh), F32)
                for j in range(8):
                    prod = lax.dot_general(
                        lhs,
                        split_buf[c * 8 + j, h],
                        (((1,), (1,)), ((), ())),
                        preferred_element_type=F32,
                    )
                    acc = jnp.where(sub == j, prod[0:8] + prod[8:16], acc)
                read_buf[eight, lanes] = acc
            return 0

        lax.fori_loop(0, seqs // 8, read_chunk, 0)

        lane = lax.broadcasted_iota(jnp.int32, pre.shape, 1)
        aux = jnp.zeros(pre.shape, F32)
        for h in range(heads):
            lanes = slice(h * dh, (h + 1) * dh)
            head = t * heads + h
            igate = jnp.sum(jnp.where(lane == head, pre, 0.0), axis=1, keepdims=True)
            fpre = jnp.sum(jnp.where(lane == head + all_heads, pre, 0.0), axis=1, keepdims=True)
            lf = jnp.minimum(fpre, 0.0) - jnp.log1p(jnp.exp(-jnp.abs(fpre)))
            stab_row = jnp.broadcast_to(stab_buf[b, h : h + 1, :], (seqs, seqs))
            diag = lax.broadcasted_iota(jnp.int32, (seqs, seqs), 0) == (
                lax.broadcasted_iota(jnp.int32, (seqs, seqs), 1)
            )
            m0 = jnp.sum(jnp.where(diag, stab_row, 0.0), axis=1, keepdims=True)
            carried = lf + m0
            m1 = jnp.maximum(carried, igate)
            stab_out[b, h : h + 1, :] = jnp.sum(jnp.where(diag, m1, 0.0), axis=0, keepdims=True)
            keep = jnp.exp(carried - m1)
            write = jnp.exp(igate - m1)
            qh, kh = query[:, lanes], key[:, lanes]
            written = write * value[:, lanes]
            n1 = keep * normer_buf[b, :, h, :] + write * kh
            value_out[b, :, lanes] = written
            normer_out[b, :, lanes] = n1
            aux = jnp.where(lane == h, keep, aux)
            numer = keep * read_buf[:, lanes] + written * jnp.sum(kh * qh, axis=1, keepdims=True)
            denom = jnp.maximum(jnp.abs(jnp.sum(n1 * qh, axis=1, keepdims=True)), 1.0)
            readout = numer / denom
            normed = readout * lax.rsqrt(
                jnp.mean(readout * readout, axis=1, keepdims=True) + EPSILON
            )
            normed = normed * head_buf[b : b + 1, lanes]
            gate = 1.0 / (1.0 + jnp.exp(-outgate[:, lanes]))
            gated_all[b, own, lanes] = (gate * normed).astype(BF16)
        aux_out[b] = aux

        spread = []
        for k in range(1, ndp):
            copy = pltpu.make_async_remote_copy(
                src_ref=gated_all.at[b, own],
                dst_ref=gated_all.at[b, own],
                send_sem=gg_send.at[b, k - 1],
                recv_sem=gg_recv.at[b, k - 1],
                device_id={"dp": lax.rem(d + k, ndp)},
                device_id_type=MESH,
            )
            copy.start()
            spread.append(copy)
        for c in spread:
            c.wait_recv()
        part = jnp.dot(gated_all[b], proj_buf[b], preferred_element_type=F32)
        out_part[...] = part
        out_stage[b] = part.astype(BF16)
        outs = []
        for k in range(1, ntp):
            dest = lax.rem(t + k, ntp)
            copy = pltpu.make_async_remote_copy(
                src_ref=out_stage.at[b, row_block(dest, rows)],
                dst_ref=out_recv.at[b, k - 1],
                send_sem=os_send.at[b, k - 1],
                recv_sem=os_recv.at[b, k - 1],
                device_id={"tp": dest},
                device_id_type=MESH,
            )
            copy.start()
            outs.append(copy)
        if b + 1 < blocks:
            split_cells(b + 1)
        for c in outs:
            c.wait_recv()
        summed = out_part[row_block(t, rows), :]
        for k in range(ntp - 1):
            summed = summed + out_recv[b, k].astype(F32)
        if b + 1 < blocks:
            current[b + 1, row_block(t, rows), :] = summed.astype(BF16)
        else:
            final_out[...] = summed.astype(BF16)
        for c in sends + spread + outs:
            c.wait_send()


def update_kernel(
    cell, value, key, aux, normer, stab_in, rows_in, cell_out, normer_out, stab_out, rows_out
):
    chunk, heads, dh = cell.shape[1], cell.shape[2], cell.shape[3]
    b = pl.program_id(0)
    here = row_block(pl.program_id(1), chunk)
    keep = aux[b, here, :]
    for h in range(heads):
        lanes = slice(h * dh, (h + 1) * dh)
        across = jnp.transpose(value[b, here, lanes])
        keys = key[b, here, lanes]
        for j in range(chunk):
            cell_out[0, j, h] = (
                keep[j : j + 1, h : h + 1] * cell[0, j, h]
                + across[:, j : j + 1] * keys[j : j + 1, :]
            )
        normer_out[0, :, h, :] = normer[b, here, lanes]
    stab_out[...] = stab_in[...]
    rows_out[...] = rows_in[...]


def origin(ndim, b, c):
    return (0,) * ndim


def per_device(ntp, ndp, *args):
    (tokens, wq, wk, wv, wo, wig, wfg, norm_gain, head_gain, proj, cell, normer, stab) = args
    blocks, width, inner = wq.shape
    all_heads = wig.shape[2]
    seqs, heads, dh = cell.shape[1], cell.shape[2], cell.shape[3]
    rows = tokens.shape[0]
    pair = 2 if ndp % 2 == 0 else 1
    ring = ndp // pair
    more = max(ring - 1, 1)
    wig, wfg, stab = (jnp.swapaxes(a, 1, 2) for a in (wig, wfg, stab))
    batch = rows * ntp
    lanes = -(-(2 * all_heads + 1) // 128) * 128
    hbm = pl.BlockSpec(memory_space=pltpu.HBM)
    dma = pltpu.SemaphoreType.DMA
    final_rows, value, key, normer_rows, aux, stab_rows = pl.pallas_call(
        functools.partial(step_kernel, ntp, ndp),
        out_shape=(
            jax.ShapeDtypeStruct(tokens.shape, BF16),
            jax.ShapeDtypeStruct((blocks, seqs, inner), F32),
            jax.ShapeDtypeStruct((blocks, seqs, inner), F32),
            jax.ShapeDtypeStruct((blocks, seqs, inner), F32),
            jax.ShapeDtypeStruct((blocks, seqs, lanes), F32),
            jax.ShapeDtypeStruct(stab.shape, F32),
        ),
        in_specs=[hbm] * 13,
        out_specs=(pl.BlockSpec(),) * 6,
        scratch_shapes=[
            pltpu.VMEM((blocks, 4, width, inner), BF16),
            pltpu.VMEM((blocks, all_heads, width), BF16),
            pltpu.VMEM((blocks, all_heads, width), BF16),
            pltpu.VMEM(proj.shape, BF16),
            pltpu.VMEM(cell.shape, F32),
            dma,
            dma((4,)),
            pltpu.VMEM(norm_gain.shape, F32),
            pltpu.VMEM(head_gain.shape, F32),
            pltpu.VMEM(normer.shape, F32),
            pltpu.VMEM(stab.shape, F32),
            pltpu.VMEM((seqs, heads, dh, 2 * dh), BF16),
            pltpu.VMEM((blocks, batch, width), BF16),
            pltpu.VMEM((blocks, batch, 4 * inner), F32),
            pltpu.VMEM((blocks, batch, lanes), F32),
            pltpu.VMEM((blocks, ring, seqs, 4 * inner), F32),
            pltpu.VMEM((blocks, ring, seqs, lanes), F32),
            pltpu.VMEM((blocks, more, seqs, 4 * inner), F32),
            pltpu.VMEM((blocks, more, seqs, lanes), F32),
            pltpu.VMEM((blocks, more, seqs, 4 * inner), F32),
            pltpu.VMEM((blocks, more, seqs, lanes), F32),
            pltpu.VMEM((seqs, inner), F32),
            pltpu.VMEM((seqs, inner), F32),
            pltpu.VMEM((blocks, batch, inner), BF16),
            pltpu.VMEM((batch, width), F32),
            pltpu.VMEM((blocks, batch, width), BF16),
            pltpu.VMEM((blocks, ntp - 1, rows, width), BF16),
            dma((blocks, 7)),
            dma((blocks,)),
            dma((blocks, ntp - 1)),
            dma((blocks, ntp - 1)),
            dma((blocks, ring)),
            dma((blocks, ring)),
            dma((blocks, ring)),
            dma((blocks, ring)),
            dma((blocks, more)),
            dma((blocks, more)),
            dma((blocks, more)),
            dma((blocks, more)),
            dma((blocks, ndp - 1)),
            dma((blocks, ndp - 1)),
            dma((blocks, ntp - 1)),
            dma((blocks, ntp - 1)),
        ],
        compiler_params=pltpu.CompilerParams(
            collective_id=0, has_side_effects=True, vmem_limit_bytes=67_043_328
        ),
    )(tokens, wq, wk, wv, wo, wig, wfg, norm_gain, head_gain, proj, cell, normer, stab)

    chunk = math.gcd(seqs, 8)
    whole_rows = pl.BlockSpec(tokens.shape, lambda b, c: (0, 0))
    whole_stab = pl.BlockSpec(stab.shape, lambda b, c: (0, 0, 0))
    cell_spec = pl.BlockSpec((1, chunk, heads, dh, dh), lambda b, c: (b, c, 0, 0, 0))
    cell_out, normer_out, stab_out, rows_out = pl.pallas_call(
        update_kernel,
        grid=(blocks, seqs // chunk),
        out_shape=(
            jax.ShapeDtypeStruct(cell.shape, F32),
            jax.ShapeDtypeStruct(normer.shape, F32),
            jax.ShapeDtypeStruct(stab.shape, F32),
            jax.ShapeDtypeStruct(tokens.shape, BF16),
        ),
        in_specs=[cell_spec]
        + [
            pl.BlockSpec(a.shape, functools.partial(origin, a.ndim))
            for a in (value, key, aux, normer_rows, stab_rows, final_rows)
        ],
        out_specs=(
            cell_spec,
            pl.BlockSpec((1, chunk, heads, dh), lambda b, c: (b, c, 0, 0)),
            whole_stab,
            whole_rows,
        ),
    )(cell, value, key, aux, normer_rows, stab_rows, final_rows)
    return rows_out, cell_out, normer_out, jnp.swapaxes(stab_out, 1, 2)


def solution(mesh):
    return jax.shard_map(
        functools.partial(per_device, mesh.shape["tp"], mesh.shape["dp"]),
        mesh=mesh,
        in_specs=(
            P("tp", "dp"),
            P(None, "dp", "tp"),
            P(None, "dp", "tp"),
            P(None, "dp", "tp"),
            P(None, "dp", "tp"),
            P(),
            P(),
            P(None, "dp"),
            P(None, "tp"),
            P(None, "tp", "dp"),
            P(None, "dp", "tp", None, None),
            P(None, "dp", "tp", None),
            P(None, "dp", "tp"),
        ),
        out_specs=(
            P("tp", "dp"),
            P(None, "dp", "tp", None, None),
            P(None, "dp", "tp", None),
            P(None, "dp", "tp"),
        ),
        check_vma=False,
    )
```

```python
import functools
import math

import jax
import jax.numpy as jnp
from jax import lax
from jax.experimental import pallas as pl
from jax.experimental.pallas import tpu as pltpu
from jax.sharding import PartitionSpec as P

EPSILON = 1e-06
F32 = jnp.float32
BF16 = jnp.bfloat16
MESH = pl.DeviceIdType.MESH


def split_axis(size):
    inner = max(f for f in range(1, math.isqrt(size) + 1) if size % f == 0)
    return size // inner, inner


def row_block(index, rows):
    return pl.ds(pl.multiple_of(index * rows, rows), rows)


def gate_dot(scaled, weight):
    return lax.dot_general(
        scaled, weight, (((1,), (1,)), ((), ())), preferred_element_type=F32
    )


def step_kernel(
    ntp,
    ndp,
    tokens,
    wq,
    wk,
    wv,
    wo,
    wig,
    wfg,
    norm_gain,
    head_gain,
    proj,
    cell,
    normer,
    stab,
    final_out,
    cell_buf,
    normer_out,
    stab_out,
    w_buf,
    ig_buf,
    fg_buf,
    proj_buf,
    written_buf,
    key_buf,
    keep_buf,
    tok_sem,
    small_sem,
    gain_buf,
    head_buf,
    normer_buf,
    stab_buf,
    split_buf,
    current,
    partial,
    gates,
    pair_recv,
    pair_gate,
    pair_sum,
    pair_gsum,
    proj_recv,
    gate_recv,
    gated_all,
    out_part,
    out_stage,
    out_recv,
    load_sem,
    cell_sem,
    ag_send,
    ag_recv,
    pr_send,
    pr_recv,
    pg_send,
    pg_recv,
    rs_send,
    rs_recv,
    gt_send,
    gt_recv,
    gg_send,
    gg_recv,
    os_send,
    os_recv,
):
    blocks = wq.shape[0]
    width, inner = wq.shape[1], wq.shape[2]
    all_heads = wig.shape[1]
    seqs, heads, dh = cell.shape[1], cell.shape[2], cell.shape[3]
    rows = tokens.shape[0]
    t = lax.axis_index("tp")
    d = lax.axis_index("dp")
    outer, side = split_axis(ntp)
    z = t // side
    x = lax.rem(t, side)

    pair = 2 if ndp % 2 == 0 else 1
    ring = ndp // pair
    y = d // pair
    core = lax.rem(d, pair)

    tok_load = pltpu.make_async_copy(tokens, current.at[0, row_block(t, rows)], tok_sem)
    tok_load.start()
    small = [
        pltpu.make_async_copy(src, dst, small_sem.at[i])
        for i, (src, dst) in enumerate(
            (
                (norm_gain, gain_buf),
                (head_gain, head_buf),
                (normer, normer_buf),
                (stab, stab_buf),
            )
        )
    ]
    loads = []
    for b in range(blocks):
        for i, w in enumerate((wq, wk, wv, wo)):
            loads.append(pltpu.make_async_copy(w.at[b], w_buf.at[b, i], load_sem.at[b, i]))
        loads.append(
            pltpu.make_async_copy(
                wig.at[b, :, row_block(d, width)], ig_buf.at[b], load_sem.at[b, 4]
            )
        )
        loads.append(
            pltpu.make_async_copy(
                wfg.at[b, :, row_block(d, width)], fg_buf.at[b], load_sem.at[b, 5]
            )
        )
        loads.append(pltpu.make_async_copy(proj.at[b], proj_buf.at[b], load_sem.at[b, 6]))
    cell_loads = [
        pltpu.make_async_copy(cell.at[b], cell_buf.at[b], cell_sem.at[b]) for b in range(blocks)
    ]
    per_block = 7
    for b in range(blocks):
        for c in loads[b * per_block : (b + 1) * per_block]:
            c.start()
        cell_loads[b].start()
        if b == 0:
            for c in small:
                c.start()

    barrier = pltpu.get_barrier_semaphore()
    for k in range(1, ntp):
        pl.semaphore_signal(
            barrier, inc=1, device_id={"tp": lax.rem(t + k, ntp)}, device_id_type=MESH
        )
    for k in range(1, ndp):
        pl.semaphore_signal(
            barrier, inc=1, device_id={"dp": lax.rem(d + k, ndp)}, device_id_type=MESH
        )
    pl.semaphore_wait(barrier, ntp - 1 + ndp - 1)
    tok_load.wait()

    def split_cells(b):
        cell_loads[b].wait()

        def one(i, _):
            for h in range(heads):
                whole = cell_buf[b, i, h]
                high = whole.astype(BF16)
                here = row_block(i, dh)
                split_buf[h, here, 0:dh] = high
                split_buf[h, here, dh : 2 * dh] = (whole - high.astype(F32)).astype(BF16)
            return 0

        lax.fori_loop(0, seqs, one, 0)

    eight = math.gcd(seqs, 8)

    def update_cells(b):
        def one(c, _):
            here = row_block(c, eight)
            keep = keep_buf[here, :]
            for h in range(heads):
                lanes = slice(h * dh, (h + 1) * dh)
                across = jnp.transpose(written_buf[here, lanes])
                keys = key_buf[here, lanes]
                for j in range(eight):
                    cell_buf[b, c * eight + j, h] = (
                        keep[j : j + 1, h : h + 1] * cell_buf[b, c * eight + j, h]
                        + across[:, j : j + 1] * keys[j : j + 1, :]
                    )
            return 0

        lax.fori_loop(0, seqs // eight, one, 0)

    def gather(b):
        buf = current.at[b]
        own_src = buf.at[row_block(t, rows)]

        def send(src, block, slot, dest):
            copy = pltpu.make_async_remote_copy(
                src_ref=src,
                dst_ref=buf.at[row_block(block, rows)],
                send_sem=ag_send.at[b, slot],
                recv_sem=ag_recv.at[b, slot],
                device_id={"tp": dest},
                device_id_type=MESH,
            )
            copy.start()
            return copy

        first, second = [], []
        for k in range(1, outer):
            dest = lax.rem(z + k, outer) * side + x
            first.append(send(own_src, t, k - 1, dest))
        for j in range(1, side):
            dest = z * side + lax.rem(x + j, side)
            second.append(send(own_src, t, outer - 1 + (j - 1) * outer, dest))
        if b == 0:
            split_cells(0)
            for c in small:
                c.wait()
        for k in range(1, outer):
            first[k - 1].wait_recv()
            block = lax.rem(z - k + outer, outer) * side + x
            for j in range(1, side):
                dest = z * side + lax.rem(x + j, side)
                second.append(
                    send(
                        buf.at[row_block(block, rows)],
                        block,
                        outer - 1 + (j - 1) * outer + k,
                        dest,
                    )
                )
        for c in second:
            c.wait_recv()
        for c in first + second:
            c.wait_send()

    for b in range(blocks):
        gather(b)
        for c in loads[b * per_block : (b + 1) * per_block]:
            c.wait()
        as_float = current[b].astype(F32)
        scaled = (as_float * gain_buf[b : b + 1, :]).astype(BF16)
        gates[b, :, 0:all_heads] = gate_dot(scaled, ig_buf[b])
        gates[b, :, all_heads : 2 * all_heads] = gate_dot(scaled, fg_buf[b])
        gates[b, :, 2 * all_heads : 2 * all_heads + 1] = jnp.sum(
            as_float * as_float, axis=1, keepdims=True
        )
        sends = []

        def send_rows(srcs, dsts, send_sems, recv_sems, slot, dest):
            started = []
            for src, dst, ss, rr in zip(srcs, dsts, send_sems, recv_sems):
                copy = pltpu.make_async_remote_copy(
                    src_ref=src,
                    dst_ref=dst,
                    send_sem=ss.at[b, slot],
                    recv_sem=rr.at[b, slot],
                    device_id={"dp": dest},
                    device_id_type=MESH,
                )
                copy.start()
                started.append(copy)
            sends.extend(started)
            return started

        for i in range(4):
            cols = slice(i * inner, (i + 1) * inner)
            partial[b, :, cols] = jnp.dot(scaled, w_buf[b, i], preferred_element_type=F32)
        paired = []
        if pair == 2:
            mate = y * pair + 1 - core
            for k in range(ring):
                slot = (k + 1) % ring
                block = row_block(lax.rem(y + slot, ring) * pair + 1 - core, seqs)
                paired.append(
                    (
                        slot,
                        send_rows(
                            (partial.at[b, block], gates.at[b, block]),
                            (pair_recv.at[b, slot], pair_gate.at[b, slot]),
                            (pr_send, pg_send),
                            (pr_recv, pg_recv),
                            slot,
                            mate,
                        ),
                    )
                )
        else:
            paired = [((k + 1) % ring, []) for k in range(ring)]
        arriving = []
        total = gate_sum = None
        for slot, copies in paired:
            for c in copies:
                c.wait_recv()
            dest = lax.rem(y + slot, ring) * pair + core
            block = row_block(dest, seqs)
            rows_sum, gsum = partial[b, block, :], gates[b, block, :]
            if copies:
                rows_sum = rows_sum + pair_recv[b, slot]
                gsum = gsum + pair_gate[b, slot]
            if slot == 0:
                total, gate_sum = rows_sum, gsum
            else:
                pair_sum[b, slot - 1] = rows_sum.astype(pair_sum.dtype)
                pair_gsum[b, slot - 1] = gsum
                arriving.append(
                    send_rows(
                        (pair_sum.at[b, slot - 1], pair_gsum.at[b, slot - 1]),
                        (proj_recv.at[b, slot - 1], gate_recv.at[b, slot - 1]),
                        (rs_send, gt_send),
                        (rs_recv, gt_recv),
                        slot - 1,
                        dest,
                    )
                )
        for k in range(ring - 1):
            for c in arriving[k]:
                c.wait_recv()
            total = total + proj_recv[b, k].astype(F32)
            gate_sum = gate_sum + gate_recv[b, k]
        own = row_block(d, seqs)
        inv_rms = lax.rsqrt(gate_sum[:, 2 * all_heads : 2 * all_heads + 1] / (width * ndp) + EPSILON)
        query = total[:, 0:inner] * inv_rms
        key = total[:, inner : 2 * inner] * inv_rms * (dh ** (-0.5))
        value = total[:, 2 * inner : 3 * inner] * inv_rms
        outgate = total[:, 3 * inner : 4 * inner] * inv_rms
        pre = gate_sum * inv_rms
        key_buf[...] = key
        wide = -(-2 * seqs // 128) * 128
        column = lax.broadcasted_iota(jnp.int32, (dh, wide), 1)
        reads = []
        for h in range(heads):
            lanes = slice(h * dh, (h + 1) * dh)
            high = query[:, lanes].astype(BF16)
            low = (query[:, lanes] - high.astype(F32)).astype(BF16)
            terms = [jnp.concatenate([a, a], 1) for a in (high, low)]
            if wide > 2 * seqs:
                terms.append(jnp.zeros((wide - 2 * seqs, 2 * dh), BF16))
            rhs = jnp.concatenate(terms, 0)
            acc = jnp.zeros((dh, wide), F32)
            for c in range(seqs // eight):
                prod = gate_dot(
                    split_buf[h, c * eight * dh : (c + 1) * eight * dh, :], rhs
                )
                for j in range(eight):
                    own_column = (column == c * eight + j) | (column == seqs + c * eight + j)
                    acc = jnp.where(own_column, prod[j * dh : (j + 1) * dh], acc)
            turned = jnp.transpose(acc)
            reads.append(turned[0:seqs] + turned[seqs : 2 * seqs])

        lane = lax.broadcasted_iota(jnp.int32, pre.shape, 1)
        aux = jnp.zeros(pre.shape, F32)
        for h in range(heads):
            lanes = slice(h * dh, (h + 1) * dh)
            head = t * heads + h
            igate = jnp.sum(jnp.where(lane == head, pre, 0.0), axis=1, keepdims=True)
            fpre = jnp.sum(jnp.where(lane == head + all_heads, pre, 0.0), axis=1, keepdims=True)
            lf = jnp.minimum(fpre, 0.0) - jnp.log1p(jnp.exp(-jnp.abs(fpre)))
            stab_row = jnp.broadcast_to(stab_buf[b, h : h + 1, :], (seqs, seqs))
            diag = lax.broadcasted_iota(jnp.int32, (seqs, seqs), 0) == (
                lax.broadcasted_iota(jnp.int32, (seqs, seqs), 1)
            )
            m0 = jnp.sum(jnp.where(diag, stab_row, 0.0), axis=1, keepdims=True)
            carried = lf + m0
            m1 = jnp.maximum(carried, igate)
            stab_out[b, h : h + 1, :] = jnp.sum(jnp.where(diag, m1, 0.0), axis=0, keepdims=True)
            keep = jnp.exp(carried - m1)
            write = jnp.exp(igate - m1)
            qh, kh = query[:, lanes], key[:, lanes]
            written = write * value[:, lanes]
            n1 = keep * normer_buf[b, :, h, :] + write * kh
            written_buf[:, lanes] = written
            normer_out[b, :, h, :] = n1
            aux = jnp.where(lane == h, keep, aux)
            numer = keep * reads[h] + written * jnp.sum(kh * qh, axis=1, keepdims=True)
            denom = jnp.maximum(jnp.abs(jnp.sum(n1 * qh, axis=1, keepdims=True)), 1.0)
            readout = numer / denom
            normed = readout * lax.rsqrt(
                jnp.mean(readout * readout, axis=1, keepdims=True) + EPSILON
            )
            normed = normed * head_buf[b : b + 1, lanes]
            gate = 1.0 / (1.0 + jnp.exp(-outgate[:, lanes]))
            gated_all[b, own, lanes] = (gate * normed).astype(BF16)
        keep_buf[...] = aux

        spread = []
        for k in range(1, ndp):
            copy = pltpu.make_async_remote_copy(
                src_ref=gated_all.at[b, own],
                dst_ref=gated_all.at[b, own],
                send_sem=gg_send.at[b, k - 1],
                recv_sem=gg_recv.at[b, k - 1],
                device_id={"dp": lax.rem(d + k, ndp)},
                device_id_type=MESH,
            )
            copy.start()
            spread.append(copy)
        for c in spread:
            c.wait_recv()
        part = jnp.dot(gated_all[b], proj_buf[b], preferred_element_type=F32)
        out_part[...] = part
        out_stage[b] = part.astype(BF16)
        outs = []
        for k in range(1, ntp):
            dest = lax.rem(t + k, ntp)
            copy = pltpu.make_async_remote_copy(
                src_ref=out_stage.at[b, row_block(dest, rows)],
                dst_ref=out_recv.at[b, k - 1],
                send_sem=os_send.at[b, k - 1],
                recv_sem=os_recv.at[b, k - 1],
                device_id={"tp": dest},
                device_id_type=MESH,
            )
            copy.start()
            outs.append(copy)
        update_cells(b)
        if b + 1 < blocks:
            split_cells(b + 1)
        for c in outs:
            c.wait_recv()
        summed = out_part[row_block(t, rows), :]
        for k in range(ntp - 1):
            summed = summed + out_recv[b, k].astype(F32)
        if b + 1 < blocks:
            current[b + 1, row_block(t, rows), :] = summed.astype(BF16)
        else:
            final_out[...] = summed.astype(BF16)
        for c in sends + spread + outs:
            c.wait_send()


def store_kernel(*refs):
    sems = refs[-1]
    half = (len(refs) - 1) // 2
    copies = [
        pltpu.make_async_copy(refs[i], refs[half + i], sems.at[i]) for i in range(half)
    ]
    for c in copies:
        c.start()
    for c in copies:
        c.wait()


def kernel_grant(*kept):
    return 67_043_328 - sum(a.size * a.dtype.itemsize for a in kept) - 65536


def per_device(ntp, ndp, *args):
    (tokens, wq, wk, wv, wo, wig, wfg, norm_gain, head_gain, proj, cell, normer, stab) = args
    blocks, width, inner = wq.shape
    all_heads = wig.shape[2]
    seqs, heads, dh = cell.shape[1], cell.shape[2], cell.shape[3]
    rows = tokens.shape[0]
    pair = 2 if ndp % 2 == 0 else 1
    ring = ndp // pair
    more = max(ring - 1, 1)
    wig, wfg, stab = (jnp.swapaxes(a, 1, 2) for a in (wig, wfg, stab))
    batch = rows * ntp
    lanes = -(-(2 * all_heads + 1) // 128) * 128
    vmem = pl.BlockSpec(memory_space=pltpu.VMEM)
    hbm = pl.BlockSpec(memory_space=pltpu.HBM)
    dma = pltpu.SemaphoreType.DMA
    results = pl.pallas_call(
        functools.partial(step_kernel, ntp, ndp),
        out_shape=(
            jax.ShapeDtypeStruct(tokens.shape, BF16),
            jax.ShapeDtypeStruct(cell.shape, F32),
            jax.ShapeDtypeStruct(normer.shape, F32),
            jax.ShapeDtypeStruct(stab.shape, F32),
        ),
        in_specs=[hbm] * 13,
        out_specs=(vmem,) * 4,
        scratch_shapes=[
            pltpu.VMEM((blocks, 4, width, inner), BF16),
            pltpu.VMEM((blocks, all_heads, width), BF16),
            pltpu.VMEM((blocks, all_heads, width), BF16),
            pltpu.VMEM(proj.shape, BF16),
            pltpu.VMEM((seqs, inner), F32),
            pltpu.VMEM((seqs, inner), F32),
            pltpu.VMEM((seqs, lanes), F32),
            dma,
            dma((4,)),
            pltpu.VMEM(norm_gain.shape, F32),
            pltpu.VMEM(head_gain.shape, F32),
            pltpu.VMEM(normer.shape, F32),
            pltpu.VMEM(stab.shape, F32),
            pltpu.VMEM((heads, seqs * dh, 2 * dh), BF16),
            pltpu.VMEM((blocks, batch, width), BF16),
            pltpu.VMEM((blocks, batch, 4 * inner), F32),
            pltpu.VMEM((blocks, batch, lanes), F32),
            pltpu.VMEM((blocks, ring, seqs, 4 * inner), F32),
            pltpu.VMEM((blocks, ring, seqs, lanes), F32),
            pltpu.VMEM((blocks, more, seqs, 4 * inner), F32),
            pltpu.VMEM((blocks, more, seqs, lanes), F32),
            pltpu.VMEM((blocks, more, seqs, 4 * inner), F32),
            pltpu.VMEM((blocks, more, seqs, lanes), F32),
            pltpu.VMEM((blocks, batch, inner), BF16),
            pltpu.VMEM((batch, width), F32),
            pltpu.VMEM((blocks, batch, width), BF16),
            pltpu.VMEM((blocks, ntp - 1, rows, width), BF16),
            dma((blocks, 7)),
            dma((blocks,)),
            dma((blocks, ntp - 1)),
            dma((blocks, ntp - 1)),
            dma((blocks, ring)),
            dma((blocks, ring)),
            dma((blocks, ring)),
            dma((blocks, ring)),
            dma((blocks, more)),
            dma((blocks, more)),
            dma((blocks, more)),
            dma((blocks, more)),
            dma((blocks, ndp - 1)),
            dma((blocks, ndp - 1)),
            dma((blocks, ntp - 1)),
            dma((blocks, ntp - 1)),
        ],
        compiler_params=pltpu.CompilerParams(
            collective_id=0, has_side_effects=True, vmem_limit_bytes=kernel_grant(cell, normer, tokens)
        ),
    )(tokens, wq, wk, wv, wo, wig, wfg, norm_gain, head_gain, proj, cell, normer, stab)

    shapes = tuple(jax.ShapeDtypeStruct(a.shape, a.dtype) for a in results)
    rows_out, cell_out, normer_out, stab_out = pl.pallas_call(
        store_kernel,
        out_shape=shapes,
        in_specs=[vmem] * 4,
        out_specs=(hbm,) * 4,
        scratch_shapes=[dma((4,))],
    )(*results)
    return rows_out, cell_out, normer_out, jnp.swapaxes(stab_out, 1, 2)


def solution(mesh):
    return jax.shard_map(
        functools.partial(per_device, mesh.shape["tp"], mesh.shape["dp"]),
        mesh=mesh,
        in_specs=(
            P("tp", "dp"),
            P(None, "dp", "tp"),
            P(None, "dp", "tp"),
            P(None, "dp", "tp"),
            P(None, "dp", "tp"),
            P(),
            P(),
            P(None, "dp"),
            P(None, "tp"),
            P(None, "tp", "dp"),
            P(None, "dp", "tp", None, None),
            P(None, "dp", "tp", None),
            P(None, "dp", "tp"),
        ),
        out_specs=(
            P("tp", "dp"),
            P(None, "dp", "tp", None, None),
            P(None, "dp", "tp", None),
            P(None, "dp", "tp"),
        ),
        check_vma=False,
    )
```
